32 devices in a mesh: sp: 16 (over z, y, x), tp: 2 (over core).
Axes of the slice: x: 2, y: 2, z: 4, core: 2. Of those that a mesh axis runs over, the one named last changes fastest.
Arguments:
- resid: bfloat16 [4096, 2048], P(('sp', 'tp')), may hold values from -3 to 3
- queries: bfloat16 [4096, 1024], P('sp', 'tp'), may hold values from -8 to 8
- keys: bfloat16 [4096, 256], P('sp', 'tp'), may hold values from -8 to 8
- values: bfloat16 [4096, 256], P('sp', 'tp'), may hold values from -6 to 6
- docs: int32 [4096], P('sp'), may hold values from 0 to 3, never falling along the last dimension, each value on 1 to 2048 neighbouring positions
- sink: float32 [8], P('tp'), may hold values from 2 to 6
- w_out: bfloat16 [1024, 2048], replicated, may hold values from -0.375 to 0.375
- norm_gain: float32 [2048], replicated, may hold values from 0.1 to 1.9
- w_gate: bfloat16 [16, 2048, 1024], P('sp', None, 'tp'), may hold values from -0.125 to 0.125
- w_up: bfloat16 [16, 2048, 1024], P('sp', None, 'tp'), may hold values from -0.125 to 0.125
- w_down: bfloat16 [16, 1024, 2048], P('sp', 'tp'), may hold values from -0.1875 to 0.1875
- expert_ids: int32 [4096, 2], P(('sp', 'tp')), may hold values from 0 to 15, all different within a row; in each aligned block of 128 rows (0 to 127, 128 to 255, ...) at most 32 rows name the same one
- route_weights: float32 [4096, 2], P(('sp', 'tp')), may hold values from 0.1 to 0.9
Outputs:
- layer_out: bfloat16 [4096, 2048], P(('sp', 'tp'))
The draws below stay inside these ranges and needn't reach their ends.
Inputs may be any that keep to these rules, and one draw needn't show every extreme that they name: `docs`: document numbers never fall along the sequence; a document holds at most 2048 positions. `expert_ids`: each row names 2 different experts. The rows of one device (aligned blocks of 256 // 2 rows) name one expert at most 32 times, and in every draw some expert is named exactly 32 times by some device.
All inputs are finite; a program needn't handle non-finite values.
Results may differ from the reference program's by a relative error of at most 0.007.
Values may be sent and summed in bfloat16 or wider, within the bound.
No kernel may reach another device: no remote copies, remote signals or barrier semaphores. Data moves between devices by JAX's collectives and lax.ppermute only.
A program may use at most 128 MiB of HBM per device.

```python
import math
import jax
import jax.numpy as jnp
import numpy as np
from jax import lax

D = 2048
QUERY_HEADS = 8
KEY_VALUE_HEADS = 2
HEAD_WIDTH = 128
WINDOW_RADIUS = 128
FF = 1024
TOP_K = 2
TOK_DEV = 256
SEQUENCE_TOKENS = 4096
EXPERTS = 16
CAP = 32
DOCS = 4
LONGEST = 2048
N_SP = 16
N_TP = 2


def query_key_pair(key):
    base = jax.random.fold_in(key, 7)
    kq, key_window = jax.random.split(base)
    keys = jnp.clip(jax.random.normal(key_window, (SEQUENCE_TOKENS, KEY_VALUE_HEADS * HEAD_WIDTH), jnp.float32), -6.0, 6.0)
    queries = jnp.clip(1.5 * jax.random.normal(kq, (SEQUENCE_TOKENS, QUERY_HEADS * HEAD_WIDTH), jnp.float32), -8.0, 8.0)
    return (queries, keys)


def draw_queries(key, part):
    return query_key_pair(key)[0].astype(jnp.bfloat16)


def draw_keys(key, part):
    return query_key_pair(key)[1].astype(jnp.bfloat16)


def levels(own_key, extent, cuts, low, largest):
    gain, own = 1.0, jax.random.fold_in(own_key, 6)
    for position, shards_of in cuts:
        steps = jnp.exp(jax.random.uniform(jax.random.fold_in(own, position), (shards_of,), jnp.float32, low / len(cuts), largest / len(cuts)))
        gain = gain * jnp.repeat(steps, extent[position] // shards_of).reshape([-1 if axis == position else 1 for axis in range(len(extent))])
    return gain


def split_up(count, total, bound, lean):
    weights = [(1 << 20) // math.isqrt(standing ** lean) + 1 for standing in range(2, count + 1)]
    spare, given = total - bound - (count - 1), [1] * (count - 1)
    while spare > 0:
        candidates = [i for i in range(count - 1) if given[i] < bound]
        pool, budget = sum([weights[i] for i in candidates]), spare
        for i in candidates:
            addition = min(bound - given[i], max(1, budget * weights[i] // pool), spare)
            given[i] = given[i] + addition
            spare = spare - addition
    return np.array([bound] + given)


def uneven(own_key, amount, total, reach, slope):
    if amount == 2:
        one = jax.random.randint(own_key, (), max(1, total - reach), min(reach, total - 1) + 1)
        return jnp.stack([one, total - one])
    tallies = jnp.asarray(split_up(amount, total, reach, slope), jnp.int32)
    pairs = (amount - 1) // 2
    giver, taker = tallies[1:1 + 2 * pairs:2], tallies[2:2 + 2 * pairs:2]
    margin = jnp.minimum(giver - 1, reach - taker)
    shifted = jax.random.randint(jax.random.fold_in(own_key, 1), (pairs,), 0, 1 << 20) % (margin + 1)
    tallies = tallies.at[1:1 + 2 * pairs:2].set(giver - shifted).at[2:2 + 2 * pairs:2].set(taker + shifted)
    return tallies[jax.random.permutation(jax.random.fold_in(own_key, 2), amount)]


def deal_out(key, own, number, rows, number_of, top, reach, slope):
    order = jax.random.permutation(key, number_of)
    crowded, ordinary = load_shares(number_of, rows * top, reach, slope, True), load_shares(number_of, rows * top, reach, slope, False)
    places = jnp.arange(number_of)

    def named(sizes, rotation):
        used = int((sizes > 0).sum())
        fixed = max(1, used // 4)
        passed = fixed + (places - fixed + rotation * (used - fixed)) % max(1, number_of - fixed)
        return jnp.zeros((number_of,), jnp.int32).at[order[jnp.where(places < fixed, places, passed)]].set(jnp.asarray(sizes, jnp.int32))

    sizes = jnp.where(number % 4 == 0, named(crowded, number // 4), named(ordinary, number - number // 4 - 1))
    mixed = jax.random.permutation(jax.random.fold_in(own, 3), number_of)
    source_of, receiver = mixed[0:number_of // 2 * 2:2], mixed[1:number_of // 2 * 2:2]
    margin = jnp.minimum(sizes[source_of] - 1, reach - sizes[receiver]) // 2
    margin = jnp.where((source_of == order[0]) | (receiver == order[0]) | (sizes[receiver] == 0), 0, jnp.maximum(margin, 0))
    passed = jax.random.randint(jax.random.fold_in(own, 4), (number_of // 2,), 0, 1 << 20) % (margin + 1)
    sizes = sizes.at[source_of].add(-passed).at[receiver].add(passed)
    members = jnp.searchsorted(jnp.cumsum(sizes), jnp.arange(rows * top), side="right").astype(jnp.int32)
    grid = members.reshape(top, rows).T
    grid = grid[jax.random.permutation(jax.random.fold_in(own, 1), rows)]
    rotation = jax.random.randint(jax.random.fold_in(own, 2), (rows, 1), 0, top)
    return jnp.take_along_axis(grid, (jnp.arange(top)[None, :] + rotation) % top, axis=1)


def load_shares(amount, total, most, slope, full):
    portions = [(1 << 20) // math.isqrt(grade ** slope) + 1 for grade in range(1, amount + 1)]
    largest = most if full else min(most, max(-(-total // amount), total * portions[0] // sum(portions)))
    least = 1 if total - largest >= amount - 1 else 0
    given, surplus = [largest] + [least] * (amount - 1), total - largest - least * (amount - 1)
    while surplus > 0:
        candidates = [i for i in range(1, amount) if given[i] < largest] or [i for i in range(1, amount) if given[i] < most]
        whole, budget = sum([portions[i] for i in candidates]), surplus
        for i in candidates:
            more = min(most - given[i], max(1, budget * portions[i] // whole), surplus)
            given[i] = given[i] + more
            surplus = surplus - more
    return np.array(given)


def normal_values(stream_key, dims, width, bound, cuts=(), kind=jnp.bfloat16):
    level = levels(stream_key, dims, cuts, -0.22, 0.18) if cuts else 1.0
    drawn = jax.random.normal(stream_key, dims, jnp.float32) * width * level
    return jnp.minimum(jnp.maximum(drawn, -bound), bound).astype(kind)


def setup_inputs(seed: int = 0) -> dict:
    seeds = jax.random.split(jax.random.key(seed), 14)
    resid = normal_values(seeds[0], (SEQUENCE_TOKENS, D), 0.5, 3.0, ((0, 32),))
    queries = draw_queries(jax.random.fold_in(seeds[13], 71), 0)
    keys = draw_keys(jax.random.fold_in(seeds[13], 71), 0)
    values = normal_values(seeds[3], (SEQUENCE_TOKENS, KEY_VALUE_HEADS * HEAD_WIDTH), 1.0, 6.0, ((0, 16), (1, 2)))
    docs = jnp.searchsorted(jnp.cumsum(uneven(seeds[4], DOCS, SEQUENCE_TOKENS, LONGEST, 2)), jnp.arange(SEQUENCE_TOKENS), side="right").astype(jnp.int32)
    sink = jnp.clip(2.0 + 4.0 * jax.random.uniform(seeds[5], (QUERY_HEADS,), jnp.float32) ** levels(seeds[5], (QUERY_HEADS,), ((0, 2),), -0.2, 0.2), 2.0, 6.0)
    w_out = normal_values(seeds[6], (QUERY_HEADS * HEAD_WIDTH, D), (QUERY_HEADS * HEAD_WIDTH // 4) ** -0.5, 0.375)
    norm_gain = jnp.clip(1.0 + 0.18 * jax.random.normal(seeds[7], (D,), jnp.float32), 0.1, 1.9)
    w_gate = normal_values(seeds[8], (EXPERTS, D, FF), D ** -0.5, 0.125, ((0, 16), (2, 2)))
    w_up = normal_values(seeds[9], (EXPERTS, D, FF), D ** -0.5, 0.125, ((0, 16), (2, 2)))
    w_down = normal_values(seeds[10], (EXPERTS, FF, D), FF ** -0.5, 0.1875, ((0, 16), (1, 2)))
    expert_ids_keys = jax.random.split(jax.random.fold_in(seeds[11], 1), SEQUENCE_TOKENS // (TOK_DEV // N_TP))
    expert_ids_turns = jax.random.permutation(jax.random.fold_in(seeds[11], 3), SEQUENCE_TOKENS // (TOK_DEV // N_TP))
    expert_ids = jax.vmap(lambda own, number: deal_out(jax.random.fold_in(seeds[11], 2), own, number, TOK_DEV // N_TP, EXPERTS, TOP_K, CAP, 2))(expert_ids_keys, expert_ids_turns).reshape((SEQUENCE_TOKENS, TOP_K))
    route_weights = jnp.clip(0.1 + 0.79999997 * jax.random.uniform(seeds[12], (SEQUENCE_TOKENS, TOP_K), jnp.float32) ** levels(seeds[12], (SEQUENCE_TOKENS, TOP_K), ((0, 32),), -0.2, 0.2), 0.1, 0.9)
    return dict(resid=resid, queries=queries, keys=keys, values=values, docs=docs, sink=sink, w_out=w_out, norm_gain=norm_gain, w_gate=w_gate, w_up=w_up, w_down=w_down, expert_ids=expert_ids, route_weights=route_weights)


eps = 1e-06

def window_band(table):
    return jnp.concatenate([table[:-2], table[1:-1], table[2:]], axis=1)

def reference(resid, queries, keys, values, docs, sink, w_out, norm_gain, w_gate, w_up, w_down, expert_ids, route_weights):
    query_blocks = SEQUENCE_TOKENS // WINDOW_RADIUS
    head_group = QUERY_HEADS // KEY_VALUE_HEADS
    query_block = queries.astype(jnp.float32).reshape(query_blocks, WINDOW_RADIUS, KEY_VALUE_HEADS, head_group, HEAD_WIDTH)
    padded_keys = jnp.pad(keys.astype(jnp.float32), ((WINDOW_RADIUS, WINDOW_RADIUS), (0, 0))).reshape(query_blocks + 2, WINDOW_RADIUS, KEY_VALUE_HEADS, HEAD_WIDTH)
    padded_values = jnp.pad(values.astype(jnp.float32), ((WINDOW_RADIUS, WINDOW_RADIUS), (0, 0))).reshape(query_blocks + 2, WINDOW_RADIUS, KEY_VALUE_HEADS, HEAD_WIDTH)
    dpad = jnp.pad(docs, (WINDOW_RADIUS, WINDOW_RADIUS), constant_values=-1).reshape(query_blocks + 2, WINDOW_RADIUS)
    kband = window_band(padded_keys)
    value_window = window_band(padded_values)
    dband = window_band(dpad)
    scores = jnp.einsum('nqhgd,nkhd->nhgqk', query_block, kband) * HEAD_WIDTH ** (-0.5)
    qpos = jnp.arange(query_blocks)[:, None] * WINDOW_RADIUS + jnp.arange(WINDOW_RADIUS)[None, :]
    kpos = (jnp.arange(query_blocks)[:, None] - 1) * WINDOW_RADIUS + jnp.arange(3 * WINDOW_RADIUS)[None, :]
    offset = kpos[:, None, :] - qpos[:, :, None]
    qdoc = docs.reshape(query_blocks, WINDOW_RADIUS)
    valid = (jnp.abs(offset) <= WINDOW_RADIUS) & (dband[:, None, :] == qdoc[:, :, None])
    valid = valid[:, None, None]
    sink_logits = sink.astype(jnp.float32).reshape(1, KEY_VALUE_HEADS, head_group, 1, 1)
    top = jnp.maximum(lax.optimization_barrier(jnp.max(jnp.where(valid, scores, -jnp.inf), axis=-1, keepdims=True)), sink_logits)
    expo = jnp.where(valid, jnp.exp(scores - top), 0.0)
    denom = lax.optimization_barrier(jnp.sum(expo, axis=-1, keepdims=True)) + jnp.exp(sink_logits - top)
    probs = lax.optimization_barrier((expo / denom).astype(jnp.bfloat16))
    attended = jnp.einsum('nhgqk,nkhd->nqhgd', probs.astype(jnp.float32), value_window).astype(jnp.bfloat16)
    attended = attended.reshape(SEQUENCE_TOKENS, QUERY_HEADS * HEAD_WIDTH)
    mixed = resid.astype(jnp.float32) + jnp.dot(attended, w_out, preferred_element_type=jnp.float32)
    normed = (mixed * lax.rsqrt(lax.optimization_barrier(jnp.mean(mixed * mixed, axis=-1, keepdims=True)) + eps) * norm_gain.astype(jnp.float32)).astype(jnp.bfloat16)
    visits = SEQUENCE_TOKENS * TOP_K
    most = N_SP * N_TP * CAP
    flat = expert_ids.reshape(visits).astype(jnp.int32)
    order = jnp.argsort(flat, stable=True).astype(jnp.int32)
    sorted_e = flat[order]
    counts = jnp.bincount(flat, length=EXPERTS).astype(jnp.int32)
    starts = (jnp.cumsum(counts) - counts).astype(jnp.int32)
    slot_sorted = sorted_e * most + jnp.arange(visits, dtype=jnp.int32) - starts[sorted_e]
    slot = jnp.zeros((visits,), jnp.int32).at[order].set(slot_sorted.astype(jnp.int32))
    owner = jnp.arange(visits, dtype=jnp.int32) // TOP_K
    table = jnp.zeros((EXPERTS * most, D), jnp.bfloat16).at[slot].set(normed[owner]).reshape(EXPERTS, most, D)

    def run(packed):
        rows, wg, wu, wd = packed
        hidden = (jax.nn.silu(jnp.dot(rows, wg, preferred_element_type=jnp.float32)) * jnp.dot(rows, wu, preferred_element_type=jnp.float32)).astype(jnp.bfloat16)
        part = FF // N_TP
        total = jnp.zeros((most, D), jnp.float32)
        for piece in range(N_TP):
            partial_value = jnp.dot(hidden[:, piece * part:(piece + 1) * part], wd[piece * part:(piece + 1) * part], preferred_element_type=jnp.float32).astype(jnp.bfloat16)
            total = total + partial_value.astype(jnp.float32)
        return total.astype(jnp.bfloat16)
    outs = lax.map(run, (table, w_gate, w_up, w_down)).reshape(EXPERTS * most, D)
    got = outs[slot].astype(jnp.float32).reshape(SEQUENCE_TOKENS, TOP_K, D)
    extra = lax.optimization_barrier(jnp.sum(route_weights.astype(jnp.float32)[:, :, None] * got, axis=1))
    return (mixed + extra).astype(jnp.bfloat16)
```

```python
import jax
import jax.numpy as jnp
from jax import lax
from jax.sharding import PartitionSpec as P

HEAD_WIDTH = 128
WINDOW_RADIUS = 128
CHUNK_ROWS = 16


eps = 1e-06


def three_parts(x):
    high = lax.reduce_precision(x, 8, 7)
    rest = x - high
    middle = lax.reduce_precision(rest, 8, 7)
    low = rest - middle
    return jnp.stack([high, middle, low]).astype(jnp.bfloat16)


def pad_rows(rows, count, width):
    return jnp.pad(rows, ((0, count - rows.shape[0]), (0, width - rows.shape[1])))


def local(
    resid,
    queries,
    keys,
    values,
    docs,
    sink,
    w_out,
    norm_gain,
    w_gate,
    w_up,
    w_down,
    expert_ids,
    route_weights,
):
    n_sp = lax.axis_size("sp")
    n_tp = lax.axis_size("tp")
    sp = lax.axis_index("sp")
    tp = lax.axis_index("tp")
    first = tp == 0
    rows_all = queries.shape[0]
    keep = rows_all // n_tp
    reach = WINDOW_RADIUS
    kv_local = keys.shape[1] // HEAD_WIDTH
    q_local = queries.shape[1] // HEAD_WIDTH
    head_group = q_local // kv_local
    total = n_sp * rows_all

    kv = jnp.concatenate([keys, values], axis=1)
    kv_width = kv.shape[1]
    pieces = queries.shape[1] // kv_width
    doc_marks = docs.astype(jnp.bfloat16)
    own_q = lax.dynamic_slice_in_dim(queries, tp * keep, keep, 0)
    their_q = lax.dynamic_slice_in_dim(queries, (1 - tp) * keep, keep, 0)
    sent = jnp.concatenate(
        [kv]
        + [their_q[:, i * kv_width : (i + 1) * kv_width] for i in range(pieces)]
        + [pad_rows(three_parts(sink), 16, kv_width)],
        axis=0,
    )
    swap = [(0, 1), (1, 0)]
    near_start = jnp.where(first, rows_all - reach, 0)
    far_start = jnp.where(first, 0, rows_all - reach)
    near = jnp.concatenate(
        [
            lax.dynamic_slice_in_dim(kv, near_start, reach, 0),
            pad_rows(lax.dynamic_slice_in_dim(doc_marks, near_start, reach, 0)[None, :], 16, kv_width),
        ],
        axis=0,
    )
    far = lax.dynamic_slice_in_dim(kv, far_start, reach, 0)
    near_pairs = [(2 * i, 2 * i + 2) for i in range(n_sp - 1)] + [
        (2 * i + 3, 2 * i + 1) for i in range(n_sp - 1)
    ]
    far_pairs = [(2 * i + 1, 2 * i + 2) for i in range(n_sp - 1)] + [
        (2 * i + 2, 2 * i + 1) for i in range(n_sp - 1)
    ]
    near = lax.ppermute(near, ("sp", "tp"), near_pairs)
    far = lax.ppermute(far, ("sp", "tp"), far_pairs)
    taken = lax.ppermute(sent, "tp", swap)

    w_gate, w_up, w_down, taken = lax.optimization_barrier((w_gate, w_up, w_down, taken))
    gates = (w_gate[0], lax.ppermute(w_gate, "tp", swap)[0])
    ups = (w_up[0], lax.ppermute(w_up, "tp", swap)[0])
    downs = (w_down[0], lax.ppermute(w_down, "tp", swap)[0])

    their_kv = taken[:rows_all]
    swapped_q = jnp.concatenate(
        [taken[rows_all + i * keep : rows_all + (i + 1) * keep] for i in range(pieces)], axis=1
    )
    parts = taken[rows_all + pieces * keep :][:3, :q_local].astype(jnp.float32)
    their_sink = parts[0] + (parts[1] + parts[2])

    def window(edge, block):
        return jnp.where(
            first, jnp.concatenate([edge, block], axis=0), jnp.concatenate([block, edge], axis=0)
        )

    own_window = window(near[:reach], kv)
    their_window = window(far, their_kv)
    doc_edge = near[reach, :reach]
    key_docs = window(doc_edge, doc_marks)
    query_docs = lax.dynamic_slice_in_dim(doc_marks, tp * keep, keep, 0)
    split = kv_local * HEAD_WIDTH
    span = own_window.shape[0]
    all_keys = jnp.concatenate([own_window[:, :split], their_window[:, :split]], axis=1)
    all_values = jnp.concatenate([own_window[:, split:], their_window[:, split:]], axis=1)
    all_keys = all_keys.reshape(span, n_tp * kv_local, HEAD_WIDTH)
    all_values = all_values.reshape(span, n_tp * kv_local, HEAD_WIDTH)
    all_queries = jnp.concatenate([own_q, swapped_q], axis=1).reshape(
        keep, n_tp * kv_local, head_group, HEAD_WIDTH
    )
    at_query = jnp.arange(keep)[:, None]
    at_key = jnp.arange(span)[None, :]
    where_key = sp * rows_all + tp * keep - reach + at_key
    valid = (
        (jnp.abs(at_key - reach - at_query) <= reach)
        & (where_key >= 0)
        & (where_key < total)
        & (key_docs[None, :] == query_docs[:, None])
    )[None, None]
    scores = jnp.einsum(
        "qhgd,khd->hgqk", all_queries, all_keys, preferred_element_type=jnp.float32
    ) * HEAD_WIDTH ** (-0.5)
    sink_logits = jnp.concatenate([sink, their_sink]).reshape(n_tp * kv_local, head_group, 1, 1)
    top = jnp.maximum(
        jnp.max(jnp.where(valid, scores, -jnp.inf), axis=-1, keepdims=True), sink_logits
    )
    expo = jnp.where(valid, jnp.exp(scores - top), 0.0)
    denom = jnp.sum(expo, axis=-1, keepdims=True) + jnp.exp(sink_logits - top)
    probs = (expo / denom).astype(jnp.bfloat16)
    attended = jnp.einsum(
        "hgqk,khd->qhgd", probs, all_values, preferred_element_type=jnp.float32
    ).astype(jnp.bfloat16)
    attended = attended.reshape(keep, n_tp * q_local * HEAD_WIDTH)
    width = q_local * HEAD_WIDTH
    attended = jnp.where(
        first, attended, jnp.concatenate([attended[:, width:], attended[:, :width]], axis=1)
    )
    mixed = resid.astype(jnp.float32) + jnp.dot(
        attended, w_out, preferred_element_type=jnp.float32
    )
    width_d = mixed.shape[1]
    normed = (
        mixed * lax.rsqrt(jnp.mean(mixed * mixed, axis=-1, keepdims=True) + eps) * norm_gain
    ).astype(jnp.bfloat16)

    top_k = expert_ids.shape[1]
    cap = rows_all * top_k // n_sp
    flat = expert_ids.reshape(-1)
    onehot = (flat[:, None] == jnp.arange(n_sp, dtype=jnp.int32)[None, :]).astype(jnp.int32)
    rank = jnp.sum((jnp.cumsum(onehot, axis=0) - onehot) * onehot, axis=1)
    chunk = CHUNK_ROWS if cap % CHUNK_ROWS == 0 else cap
    rank = rank.reshape(keep, top_k)
    slot = (rank // chunk) * (n_sp * chunk) + expert_ids * chunk + rank % chunk

    def places(piece):
        ids = jnp.arange(n_sp * chunk, dtype=jnp.int32) + piece * n_sp * chunk
        return [(slot[:, k][:, None] == ids[None, :]).astype(jnp.bfloat16) for k in range(top_k)]

    extra = [jnp.zeros((keep, width_d), jnp.float32) for _ in range(top_k)]
    landed, chosen = [], []
    for piece in range(cap // chunk):
        marks = places(piece)
        chosen.append(marks)
        outgoing = lax.dot_general(
            sum(marks), normed, (((0,), (0,)), ((), ())), preferred_element_type=jnp.float32
        ).astype(jnp.bfloat16)
        landed.append(lax.all_to_all(outgoing, "sp", split_axis=0, concat_axis=0, tiled=True))
    for piece in range(cap // chunk):
        summed = jnp.zeros((n_sp * chunk, width_d), jnp.float32)
        for gate, up, down in zip(gates, ups, downs):
            hidden = (
                jax.nn.silu(jnp.dot(landed[piece], gate, preferred_element_type=jnp.float32))
                * jnp.dot(landed[piece], up, preferred_element_type=jnp.float32)
            ).astype(jnp.bfloat16)
            partial_value = jnp.dot(hidden, down, preferred_element_type=jnp.float32)
            summed = summed + partial_value.astype(jnp.bfloat16).astype(jnp.float32)
        back = lax.all_to_all(
            summed.astype(jnp.bfloat16), "sp", split_axis=0, concat_axis=0, tiled=True
        )
        for k in range(top_k):
            extra[k] = extra[k] + jnp.dot(
                chosen[piece][k], back, preferred_element_type=jnp.float32
            )
    out = mixed
    for k in range(top_k):
        out = out + route_weights[:, k][:, None] * extra[k]
    return out.astype(jnp.bfloat16)


def solution(mesh):
    in_specs = (
        P(("sp", "tp"), None),
        P("sp", "tp"),
        P("sp", "tp"),
        P("sp", "tp"),
        P("sp"),
        P("tp"),
        P(),
        P(),
        P("sp", None, "tp"),
        P("sp", None, "tp"),
        P("sp", "tp", None),
        P(("sp", "tp"), None),
        P(("sp", "tp"), None),
    )
    out_specs = P(("sp", "tp"), None)
    return jax.shard_map(local, mesh=mesh, in_specs=in_specs, out_specs=out_specs, check_vma=False)
```

```python
import jax
import jax.numpy as jnp
from jax import lax
from jax.experimental import pallas as pl
from jax.experimental.pallas import tpu as pltpu
from jax.sharding import PartitionSpec as P


HEAD_WIDTH = 128
WINDOW_RADIUS = 128
HIDDEN_BLOCK = 256


eps = 1e-06


def three_parts(x):
    high = lax.reduce_precision(x, 8, 7)
    rest = x - high
    middle = lax.reduce_precision(rest, 8, 7)
    low = rest - middle
    return jnp.stack([high, middle, low]).astype(jnp.bfloat16)


def pad_rows(rows, count, width):
    return jnp.pad(rows, ((0, count - rows.shape[0]), (0, width - rows.shape[1])))


def expert_kernel(rows, gate0, up0, down0, gate1, up1, down1, out, acc, kept):
    step = pl.program_id(0)
    blocks = pl.num_programs(0) // 2

    def product(gate, up, down):
        x = rows[...]
        g = jnp.dot(x, gate[...], preferred_element_type=jnp.float32)
        u = jnp.dot(x, up[...], preferred_element_type=jnp.float32)
        hidden = (g * lax.logistic(g) * u).astype(jnp.bfloat16)
        return jnp.dot(hidden, down[...], preferred_element_type=jnp.float32)

    @pl.when((step == 0) | (step == blocks))
    def _():
        acc[...] = jnp.zeros_like(acc)

    @pl.when(step < blocks)
    def _():
        acc[...] += product(gate0, up0, down0)

    @pl.when(step >= blocks)
    def _():
        acc[...] += product(gate1, up1, down1)

    @pl.when(step == blocks - 1)
    def _():
        kept[...] = acc[...].astype(jnp.bfloat16)

    @pl.when(step == 2 * blocks - 1)
    def _():
        last = acc[...].astype(jnp.bfloat16).astype(jnp.float32)
        out[...] = (kept[...].astype(jnp.float32) + last).astype(jnp.bfloat16)


def expert(rows, gates, ups, downs):
    count, width = rows.shape
    units = gates[0].shape[1]
    block = min(HIDDEN_BLOCK, units)
    blocks = units // block

    def wide(half):
        at = (lambda i: (0, jnp.minimum(i, blocks - 1))) if half == 0 else (
            lambda i: (0, jnp.maximum(i - blocks, 0))
        )
        return pl.BlockSpec((width, block), at)

    def tall(half):
        at = (lambda i: (jnp.minimum(i, blocks - 1), 0)) if half == 0 else (
            lambda i: (jnp.maximum(i - blocks, 0), 0)
        )
        return pl.BlockSpec((block, width), at)

    whole = pl.BlockSpec((count, width), lambda i: (0, 0))
    return pl.pallas_call(
        expert_kernel,
        grid=(2 * blocks,),
        in_specs=[whole, wide(0), wide(0), tall(0), wide(1), wide(1), tall(1)],
        out_specs=whole,
        out_shape=jax.ShapeDtypeStruct((count, width), jnp.bfloat16),
        scratch_shapes=[
            pltpu.VMEM((count, width), jnp.float32),
            pltpu.VMEM((count, width), jnp.bfloat16),
        ],
        compiler_params=pltpu.CompilerParams(
            dimension_semantics=("arbitrary",), vmem_limit_bytes=40 * 1024 * 1024
        ),
        cost_estimate=pl.CostEstimate(
            flops=12 * count * width * units,
            transcendentals=2 * count * units,
            bytes_accessed=12 * width * units + 4 * count * width,
        ),
        name="expert",
    )(rows, gates[0], ups[0], downs[0], gates[1], ups[1], downs[1])


def local(
    resid,
    queries,
    keys,
    values,
    docs,
    sink,
    w_out,
    norm_gain,
    w_gate,
    w_up,
    w_down,
    expert_ids,
    route_weights,
):
    n_sp = lax.axis_size("sp")
    n_tp = lax.axis_size("tp")
    sp = lax.axis_index("sp")
    tp = lax.axis_index("tp")
    first = tp == 0
    rows_all = queries.shape[0]
    keep = rows_all // n_tp
    reach = WINDOW_RADIUS
    kv_local = keys.shape[1] // HEAD_WIDTH
    q_local = queries.shape[1] // HEAD_WIDTH
    head_group = q_local // kv_local
    total = n_sp * rows_all

    kv = jnp.concatenate([keys, values], axis=1)
    kv_width = kv.shape[1]
    pieces = queries.shape[1] // kv_width
    doc_marks = docs.astype(jnp.bfloat16)
    own_q = lax.dynamic_slice_in_dim(queries, tp * keep, keep, 0)
    their_q = lax.dynamic_slice_in_dim(queries, (1 - tp) * keep, keep, 0)
    sent = jnp.concatenate(
        [kv]
        + [their_q[:, i * kv_width : (i + 1) * kv_width] for i in range(pieces)]
        + [pad_rows(three_parts(sink), 16, kv_width)],
        axis=0,
    )
    swap = [(0, 1), (1, 0)]
    near_start = jnp.where(first, rows_all - reach, 0)
    far_start = jnp.where(first, 0, rows_all - reach)
    near = jnp.concatenate(
        [
            lax.dynamic_slice_in_dim(kv, near_start, reach, 0),
            pad_rows(lax.dynamic_slice_in_dim(doc_marks, near_start, reach, 0)[None, :], 16, kv_width),
        ],
        axis=0,
    )
    far = lax.dynamic_slice_in_dim(kv, far_start, reach, 0)
    near_pairs = [(2 * i, 2 * i + 2) for i in range(n_sp - 1)] + [
        (2 * i + 3, 2 * i + 1) for i in range(n_sp - 1)
    ]
    far_pairs = [(2 * i + 1, 2 * i + 2) for i in range(n_sp - 1)] + [
        (2 * i + 2, 2 * i + 1) for i in range(n_sp - 1)
    ]
    near = lax.ppermute(near, ("sp", "tp"), near_pairs)
    far = lax.ppermute(far, ("sp", "tp"), far_pairs)
    taken = lax.ppermute(sent, "tp", swap)

    w_gate, w_up, w_down, taken = lax.optimization_barrier((w_gate, w_up, w_down, taken))
    gates = (w_gate[0], lax.ppermute(w_gate, "tp", swap)[0])
    ups = (w_up[0], lax.ppermute(w_up, "tp", swap)[0])
    downs = (w_down[0], lax.ppermute(w_down, "tp", swap)[0])

    their_kv = taken[:rows_all]
    swapped_q = jnp.concatenate(
        [taken[rows_all + i * keep : rows_all + (i + 1) * keep] for i in range(pieces)], axis=1
    )
    parts = taken[rows_all + pieces * keep :][:3, :q_local].astype(jnp.float32)
    their_sink = parts[0] + (parts[1] + parts[2])

    def window(edge, block):
        return jnp.where(
            first, jnp.concatenate([edge, block], axis=0), jnp.concatenate([block, edge], axis=0)
        )

    own_window = window(near[:reach], kv)
    their_window = window(far, their_kv)
    doc_edge = near[reach, :reach]
    key_docs = window(doc_edge, doc_marks)
    query_docs = lax.dynamic_slice_in_dim(doc_marks, tp * keep, keep, 0)
    split = kv_local * HEAD_WIDTH
    span = own_window.shape[0]
    all_keys = jnp.concatenate([own_window[:, :split], their_window[:, :split]], axis=1)
    all_values = jnp.concatenate([own_window[:, split:], their_window[:, split:]], axis=1)
    all_keys = all_keys.reshape(span, n_tp * kv_local, HEAD_WIDTH)
    all_values = all_values.reshape(span, n_tp * kv_local, HEAD_WIDTH)
    all_queries = jnp.concatenate([own_q, swapped_q], axis=1).reshape(
        keep, n_tp * kv_local, head_group, HEAD_WIDTH
    )
    at_query = jnp.arange(keep)[:, None]
    at_key = jnp.arange(span)[None, :]
    where_key = sp * rows_all + tp * keep - reach + at_key
    valid = (
        (jnp.abs(at_key - reach - at_query) <= reach)
        & (where_key >= 0)
        & (where_key < total)
        & (key_docs[None, :] == query_docs[:, None])
    )[None, None]
    scores = jnp.einsum(
        "qhgd,khd->hgqk", all_queries, all_keys, preferred_element_type=jnp.float32
    ) * HEAD_WIDTH ** (-0.5)
    sink_logits = jnp.concatenate([sink, their_sink]).reshape(n_tp * kv_local, head_group, 1, 1)
    top = jnp.maximum(
        jnp.max(jnp.where(valid, scores, -jnp.inf), axis=-1, keepdims=True), sink_logits
    )
    expo = jnp.where(valid, jnp.exp(scores - top), 0.0)
    denom = jnp.sum(expo, axis=-1, keepdims=True) + jnp.exp(sink_logits - top)
    probs = (expo / denom).astype(jnp.bfloat16)
    attended = jnp.einsum(
        "hgqk,khd->qhgd", probs, all_values, preferred_element_type=jnp.float32
    ).astype(jnp.bfloat16)
    attended = attended.reshape(keep, n_tp * q_local * HEAD_WIDTH)
    width = q_local * HEAD_WIDTH
    attended = jnp.where(
        first, attended, jnp.concatenate([attended[:, width:], attended[:, :width]], axis=1)
    )
    mixed = resid.astype(jnp.float32) + jnp.dot(
        attended, w_out, preferred_element_type=jnp.float32
    )
    normed = (
        mixed * lax.rsqrt(jnp.mean(mixed * mixed, axis=-1, keepdims=True) + eps) * norm_gain
    ).astype(jnp.bfloat16)

    top_k = expert_ids.shape[1]
    cap = rows_all * top_k // n_sp
    flat = expert_ids.reshape(-1)
    onehot = (flat[:, None] == jnp.arange(n_sp, dtype=jnp.int32)[None, :]).astype(jnp.int32)
    rank = jnp.sum((jnp.cumsum(onehot, axis=0) - onehot) * onehot, axis=1)
    slot = expert_ids * cap + rank.reshape(keep, top_k)

    half = n_sp // 2
    groups = [list(range(half)), list(range(half, n_sp))]
    across = [(i, (i + half) % n_sp) for i in range(n_sp)]
    table = jnp.concatenate([slot.astype(jnp.float32).T, route_weights.T], axis=0)
    their_table = lax.ppermute(table, "sp", across)
    base = (sp // half) * half * cap
    ids = jnp.arange(half * cap, dtype=jnp.int32)[None, :] + base

    def exchange(rows):
        return lax.all_to_all(
            rows, "sp", split_axis=0, concat_axis=0, axis_index_groups=groups, tiled=True
        )

    def dispatch(rows, entries):
        places = entries[:top_k].astype(jnp.int32)
        marks = [(places[k][:, None] == ids).astype(jnp.bfloat16) for k in range(top_k)]
        outgoing = lax.dot_general(
            sum(marks), rows, (((0,), (0,)), ((), ())), preferred_element_type=jnp.float32
        ).astype(jnp.bfloat16)
        return marks, exchange(outgoing)

    def combine(back, marks, entries):
        return sum(
            entries[top_k + k][:, None]
            * jnp.dot(marks[k], back, preferred_element_type=jnp.float32)
            for k in range(top_k)
        )

    crossed = lax.ppermute(normed, "sp", across)
    marks, landed = dispatch(normed, table)
    crossed, landed = lax.optimization_barrier((crossed, landed))
    their_marks, their_landed = dispatch(crossed, their_table)
    made = expert(landed, gates, ups, downs)
    back = exchange(made)
    their_made = expert(their_landed, gates, ups, downs)
    their_back = exchange(their_made)
    sums = combine(their_back, their_marks, their_table).astype(jnp.bfloat16)
    home = lax.ppermute(sums, "sp", across)
    out = mixed + combine(back, marks, table) + home.astype(jnp.float32)
    return out.astype(jnp.bfloat16)


def solution(mesh):
    in_specs = (
        P(("sp", "tp"), None),
        P("sp", "tp"),
        P("sp", "tp"),
        P("sp", "tp"),
        P("sp"),
        P("tp"),
        P(),
        P(),
        P("sp", None, "tp"),
        P("sp", None, "tp"),
        P("sp", "tp", None),
        P(("sp", "tp"), None),
        P(("sp", "tp"), None),
    )
    out_specs = P(("sp", "tp"), None)
    return jax.shard_map(local, mesh=mesh, in_specs=in_specs, out_specs=out_specs, check_vma=False)
```
